32 devices in a mesh: gr: 2 (over x), sp: 8 (over z, y), tp: 2 (over core).
Axes of the slice: x: 2, y: 2, z: 4, core: 2. Of those that a mesh axis runs over, the one named last changes fastest.
Arguments:
- prompt: bfloat16 [128, 128, 1024], P('gr', 'sp'), parts along dimension 0, may hold values from -6 to 6
- w_key: bfloat16 [1024, 8, 128], P(None, 'tp'), may hold values from -0.1875 to 0.1875
- w_value: bfloat16 [1024, 8, 128], P(None, 'tp'), may hold values from -0.1875 to 0.1875
- w_in_gate: bfloat16 [2, 1024, 8], P(None, None, 'tp'), may hold values from -0.1875 to 0.1875
- w_forget_gate: bfloat16 [2, 1024, 8], P(None, None, 'tp'), may hold values from -0.1875 to 0.1875
- in_bias: float32 [2, 8], P(None, 'tp'), may hold values from -6 to 0, as said below
- forget_bias: float32 [2, 8], P(None, 'tp'), may hold values from 1 to 10, as said below
- query: bfloat16 [128, 8, 128], P(('gr', 'sp'), 'tp'), parts along dimension 0, may hold values from -6 to 6
- w_out: bfloat16 [8, 128, 1024], P('tp'), may hold values from -0.5 to 0.5
Outputs:
- memory: bfloat16 [2, 128, 8, 128, 128], P(None, ('gr', 'sp'), 'tp'), parts along dimension 1
- normalizer: float32 [2, 128, 8, 128], P(None, ('gr', 'sp'), 'tp'), parts along dimension 1
- stabilizer: float32 [2, 128, 8], P(None, ('gr', 'sp'), 'tp'), parts along dimension 1
- read: bfloat16 [128, 1024], P(('gr', 'sp'), 'tp'), parts along dimension 0
The draws below stay inside these ranges and needn't reach their ends.
There are 2 independent parts, one for each index of `gr`. The reference program is written for one: setup_inputs(seed, part) draws one part's arguments, and reference() takes and returns one part's arrays. A program takes and returns all parts, laid end to end along the dimension named above; an argument that names none is the same for every part. Nothing has to cross between parts.
Inputs may be any that keep to these rules, and one draw needn't show every extreme that they name: forget_bias lies between 1 and 10; the per-head share of memory kept over the whole prompt is spread between a few and some ninety percent. in_bias lies between -6 and 0.
All inputs are finite; a program needn't handle non-finite values.
Results may differ from the reference program's by a relative error of at most 0.015.
Values may be sent and summed in bfloat16 or wider, within the bound.
A program may use at most 64 MiB of HBM per device.

```python
import math
import jax
import jax.numpy as jnp
from jax import lax

D = 1024
HEADS = 8
HEAD_DIM = 128
SEQS = 64
SEQ_LEN = 128


def draw_forget_bias(key, part):
    kept_share = jnp.exp(jax.random.uniform(key, (2, HEADS), jnp.float32, math.log(0.05), math.log(0.9)))
    chain_loss = -jnp.log(kept_share) / 1.65
    return -jnp.log(jnp.expm1(chain_loss / SEQ_LEN))


def draw_in_bias(key, part):
    centre = -0.5 * math.log(SEQ_LEN) - 1.0
    offset = jax.random.uniform(key, (2, HEADS), jnp.float32, -1.0, 1.0)
    return offset + centre


def block_scale(stream_key, dims, shards, smallest, high):
    loudness, own = 1.0, jax.random.fold_in(stream_key, 6)
    for position, shards_of in shards:
        steps = jnp.exp(jax.random.uniform(jax.random.fold_in(own, position), (shards_of,), jnp.float32, smallest / len(shards), high / len(shards)))
        loudness = loudness * jnp.repeat(steps, dims[position] // shards_of).reshape([-1 if axis == position else 1 for axis in range(len(dims))])
    return loudness


def gaussian(key, extent, scale, reach, pieces=(), kind=jnp.bfloat16):
    loudness = block_scale(key, extent, pieces, -0.22, 0.18) if pieces else 1.0
    array = jax.random.normal(key, extent, jnp.float32) * scale * loudness
    return jnp.minimum(jnp.maximum(array, -reach), reach).astype(kind)


def setup_inputs(seed: int = 0, part: int = 0) -> dict:
    keys = jax.random.split(jax.random.key(seed), 10)
    part_keys = jax.random.split(jax.random.fold_in(keys[9], part), 10)
    prompt = gaussian(part_keys[0], (SEQS, SEQ_LEN, D), 1.0, 6.0, ((1, 8),))
    w_key = gaussian(keys[1], (D, HEADS, HEAD_DIM), D ** -0.5, 0.1875, ((1, 2),))
    w_value = gaussian(keys[2], (D, HEADS, HEAD_DIM), D ** -0.5, 0.1875, ((1, 2),))
    w_in_gate = gaussian(keys[3], (2, D, HEADS), D ** -0.5, 0.1875, ((2, 2),))
    w_forget_gate = gaussian(keys[4], (2, D, HEADS), D ** -0.5, 0.1875, ((2, 2),))
    in_bias = draw_in_bias(jax.random.fold_in(keys[9], 71), part)
    forget_bias = draw_forget_bias(jax.random.fold_in(keys[9], 71), part)
    query = gaussian(part_keys[7], (SEQS, HEADS, HEAD_DIM), 1.0, 6.0, ((0, 8), (1, 2)))
    w_out = gaussian(keys[8], (HEADS, HEAD_DIM, D), (HEADS * HEAD_DIM // 9) ** -0.5, 0.5, ((0, 2),))
    return dict(prompt=prompt, w_key=w_key, w_value=w_value, w_in_gate=w_in_gate, w_forget_gate=w_forget_gate, in_bias=in_bias, forget_bias=forget_bias, query=query, w_out=w_out)


highest = lax.Precision.HIGHEST


def summary(scaled, float_values, in_log, forget_log, backward):
    total_forget = jnp.sum(forget_log, axis=1)
    running = jnp.cumsum(forget_log, axis=1)
    if backward:
        log_weight = in_log + running - forget_log
    else:
        log_weight = in_log + total_forget[:, None, :] - running
    stable = jnp.maximum(total_forget, jnp.max(log_weight, axis=1))
    weight = jnp.exp(log_weight - stable[:, None, :])
    weighted = scaled * weight[..., None]
    memory = jnp.einsum('bshd,bshe->bhde', weighted, float_values, precision=highest)
    normal = jnp.sum(weighted, axis=1)
    return memory, normal, stable


def read_out(memory_bf, normal, stable, query_f):
    cells = memory_bf.astype(jnp.float32)
    numerator = jnp.sum(query_f[..., :, None] * cells, axis=-2)
    denominator = jnp.sum(query_f * normal, axis=-1)
    floor_value = jnp.maximum(jnp.maximum(jnp.abs(denominator), jnp.exp(-stable)), 1.0)
    return numerator / floor_value[..., None]


def reference(prompt, w_key, w_value, w_in_gate, w_forget_gate, in_bias, forget_bias, query, w_out):
    token_rows = prompt.astype(jnp.float32)
    key_rows = jnp.einsum('bsd,dhe->bshe', token_rows, w_key.astype(jnp.float32), precision=highest).astype(jnp.bfloat16)
    value_rows = jnp.einsum('bsd,dhe->bshe', token_rows, w_value.astype(jnp.float32), precision=highest).astype(jnp.bfloat16)
    in_pre = jnp.einsum('bsd,gdh->bsgh', token_rows, w_in_gate.astype(jnp.float32), precision=highest) + in_bias
    forget_pre = jnp.einsum('bsd,gdh->bsgh', token_rows, w_forget_gate.astype(jnp.float32), precision=highest) + forget_bias
    scaled = key_rows.astype(jnp.float32) * (key_rows.shape[-1] ** -0.5)
    float_values = value_rows.astype(jnp.float32)
    query_f = query.astype(jnp.float32)
    memories = []
    normals = []
    stables = []
    reads = []
    for course in range(2):
        memory, normal, stable = summary(scaled, float_values, in_pre[:, :, course, :],
                                         jax.nn.log_sigmoid(forget_pre[:, :, course, :]), course == 1)
        memory_bf = memory.astype(jnp.bfloat16)
        memories.append(memory_bf)
        normals.append(normal)
        stables.append(stable)
        reads.append(read_out(memory_bf, normal, stable, query_f))
    hidden = (reads[0] + reads[1]).astype(jnp.bfloat16)
    read = jnp.einsum('bhd,hde->be', hidden.astype(jnp.float32), w_out.astype(jnp.float32), precision=highest).astype(jnp.bfloat16)
    return (jnp.stack(memories), jnp.stack(normals), jnp.stack(stables), read)
```

```python
import functools

import jax
import jax.numpy as jnp
from jax import lax
from jax.experimental import pallas as pl
from jax.experimental.pallas import tpu as pltpu
from jax.sharding import PartitionSpec as P

MESH = pl.DeviceIdType.MESH
F32 = jnp.float32
BF16 = jnp.bfloat16


def nt(a, b):
    return lax.dot_general(a, b, (((1,), (1,)), ((), ())), preferred_element_type=F32)


def kernel(
    n, tpn, heads, width, gates,
    prompt, wkt_hbm, wv_hbm, wo_hbm, bias, query,
    mem_out, norm_out, stab_out, read_out,
    xbuf, wkt, wv, wo, membuf, hid, stabs, parts, got,
    wsem, lsem, ssem, rsem, fsend, frecv, osem, xsend, xrecv,
):
    sp = lax.axis_index("sp")
    tp = lax.axis_index("tp")
    seqs, length, _ = xbuf.shape
    rounds = seqs // tpn
    block = length // n
    order = sorted(range(1, n), key=lambda k: abs(k - n / 2))

    barrier = pltpu.get_barrier_semaphore()
    for k in order:
        pl.semaphore_signal(
            barrier, inc=1, device_id={"sp": lax.rem(sp + k, n)}, device_id_type=MESH
        )
    for j in range(1, tpn):
        pl.semaphore_signal(
            barrier, inc=1, device_id={"tp": lax.rem(tp + j, tpn)}, device_id_type=MESH
        )

    weights = [
        pltpu.make_async_copy(wkt_hbm, wkt, wsem.at[0]),
        pltpu.make_async_copy(wv_hbm, wv, wsem.at[1]),
        pltpu.make_async_copy(wo_hbm, wo, wsem.at[2]),
    ]
    rows = pl.ds(pl.multiple_of(sp * block, block), block)

    def own(r):
        q = tp * rounds + r
        return pltpu.make_async_copy(prompt.at[sp * seqs + q], xbuf.at[q, rows], lsem.at[r])

    def send(r, k):
        q = tp * rounds + r
        dest = lax.rem(sp + k, n)
        return pltpu.make_async_remote_copy(
            src_ref=prompt.at[dest * seqs + q],
            dst_ref=xbuf.at[q, rows],
            send_sem=ssem.at[r, k],
            recv_sem=rsem.at[r, k],
            device_id={"sp": dest},
            device_id_type=MESH,
        )

    def forward(r, j):
        q = tp * rounds + r
        return pltpu.make_async_remote_copy(
            src_ref=xbuf.at[q],
            dst_ref=xbuf.at[q],
            send_sem=fsend.at[r, j],
            recv_sem=frecv.at[r, j],
            device_id={"tp": lax.rem(tp + j, tpn)},
            device_id_type=MESH,
        )

    def out(g, q):
        return pltpu.make_async_copy(membuf.at[g, q], mem_out.at[g, q], osem.at[g, q])

    pl.semaphore_wait(barrier, n - 1 + tpn - 1)
    for r in range(rounds):
        for k in order:
            send(r, k).start()
    for copy in weights:
        copy.start()
    for r in range(rounds):
        own(r).start()
    stabs[...] = jnp.zeros_like(stabs)
    for copy in weights:
        copy.wait()

    tri = (
        lax.broadcasted_iota(jnp.int32, (length, length), 0)
        <= lax.broadcasted_iota(jnp.int32, (length, length), 1)
    ).astype(F32)
    ahead = lax.broadcasted_iota(jnp.int32, (gates, length), 0) < heads
    lane = lax.broadcasted_iota(jnp.int32, (gates, stabs.shape[1]), 1)
    pick = lax.broadcasted_iota(jnp.int32, (16, length), 0)
    key_rows = heads * width

    def compute(q):
        x = xbuf[q]
        kt = nt(wkt[...], x)
        values = jnp.dot(x, wv[...], preferred_element_type=F32).astype(BF16)
        pre = kt[key_rows:] + bias[...]
        keys = kt[:key_rows].astype(BF16)
        in_log, forget_pre = pre[:gates], pre[gates:]
        forget = jnp.minimum(forget_pre, 0.0) - jnp.log1p(jnp.exp(-jnp.abs(forget_pre)))
        running = jnp.dot(
            forget, tri, preferred_element_type=F32, precision=lax.Precision.HIGHEST
        )
        total = jnp.sum(forget, axis=1, keepdims=True)
        log_weight = in_log + jnp.where(ahead, total - running, running - forget)
        stable = jnp.maximum(total, jnp.max(log_weight, axis=1, keepdims=True))
        weight = jnp.exp(log_weight - stable) * width ** (-0.5)
        floor = jnp.maximum(jnp.exp(-stable), 1.0)
        stabs[...] = jnp.where(lane == q, stable, stabs[...])
        high = weight.astype(BF16).astype(F32)
        split = jnp.concatenate([high, weight - high], axis=0).astype(BF16)
        queries = query[q]
        for h in range(heads):
            head = keys[h * width : (h + 1) * width]
            head_f = head.astype(F32)
            w0, w1 = weight[h : h + 1], weight[heads + h : heads + h + 1]
            scores = jnp.dot(queries, head, preferred_element_type=F32)[h : h + 1]
            q0, q1 = scores * w0, scores * w1
            both = jnp.where(lax.rem(pick, 2) == 0, q0, q1)
            top = both.astype(BF16).astype(F32)
            tail = jnp.where(pick < 2, top, jnp.where(pick < 4, both - top, 0.0)).astype(BF16)
            lhs = jnp.concatenate(
                [(head_f * w0).astype(BF16), (head_f * w1).astype(BF16), tail], axis=0
            )
            res = jnp.dot(
                lhs, values[:, h * width : (h + 1) * width], preferred_element_type=F32
            )
            membuf[0, q, h] = res[:width].astype(BF16)
            membuf[1, q, h] = res[width : 2 * width].astype(BF16)
            normal = nt(split, head)
            normal = normal[:gates] + normal[gates:]
            norm_out[0, q, h : h + 1] = normal[h : h + 1]
            norm_out[1, q, h : h + 1] = normal[heads + h : heads + h + 1]
            last = res[2 * width :]
            d0 = jnp.abs(jnp.sum(q0, axis=1, keepdims=True))
            d1 = jnp.abs(jnp.sum(q1, axis=1, keepdims=True))
            f0, f1 = floor[h : h + 1], floor[heads + h : heads + h + 1]
            hid[q, :, h * width : (h + 1) * width] = (
                (last[0:1] + last[2:3]) / jnp.maximum(d0, f0)
                + (last[1:2] + last[3:4]) / jnp.maximum(d1, f1)
            )
        for g in range(2):
            out(g, q).start()

    def turn(r, carry):
        own(r).wait()
        for k in order:
            send(r, k).wait_recv()
        for j in range(1, tpn):
            forward(r, j).start()
        compute(tp * rounds + r)
        for j in range(1, tpn):
            forward(r, j).wait_recv()
            compute(lax.rem(tp + tpn - j, tpn) * rounds + r)
        return carry

    lax.fori_loop(0, rounds, turn, 0)

    terms = jnp.dot(hid[:, 0, :].astype(BF16), wo[...], preferred_element_type=F32)
    share = terms.shape[1] // tpn
    for t in range(tpn):
        parts[t] = terms[:, t * share : (t + 1) * share]

    def give(j):
        peer = lax.rem(tp + j, tpn)
        return pltpu.make_async_remote_copy(
            src_ref=parts.at[peer],
            dst_ref=got.at[j],
            send_sem=xsend.at[j],
            recv_sem=xrecv.at[j],
            device_id={"tp": peer},
            device_id_type=MESH,
        )

    for j in range(1, tpn):
        give(j).start()
    turned = jnp.transpose(stabs[...])
    for g in range(2):
        stab_out[g] = turned[:seqs, g * heads : (g + 1) * heads]
    for r in range(rounds):
        for k in order:
            send(r, k).wait_send()
        for j in range(1, tpn):
            forward(r, j).wait_send()
    for g in range(2):
        for q in range(seqs):
            out(g, q).wait()
    total = parts[tp]
    for j in range(1, tpn):
        give(j).wait()
        total = total + got[j]
    read_out[...] = total.astype(BF16)


def solution(mesh):
    n, tpn = mesh.shape["sp"], mesh.shape["tp"]

    def body(prompt, w_key, w_value, w_in_gate, w_forget_gate, in_bias, forget_bias, query, w_out):
        depth, heads, width = w_key.shape
        seqs = prompt.shape[0] // n
        length = prompt.shape[1] * n
        rounds = seqs // tpn
        gates = -(-2 * heads // 8) * 8
        pad = gates - 2 * heads

        def gate_rows(w):
            return jnp.pad(w.transpose(0, 2, 1).reshape(2 * heads, depth), ((0, pad), (0, 0)))

        def bias_rows(b):
            return jnp.pad(b.reshape(2 * heads), (0, pad))

        wkt = jnp.concatenate(
            [
                w_key.transpose(1, 2, 0).reshape(heads * width, depth),
                gate_rows(w_in_gate),
                gate_rows(w_forget_gate),
            ]
        )
        wv = w_value.reshape(depth, heads * width)
        wo = w_out.reshape(heads * width, -1)
        bias = jnp.concatenate([bias_rows(in_bias), bias_rows(forget_bias)])[:, None]
        bias = jnp.broadcast_to(bias, (2 * gates, length))
        columns = wo.shape[1]
        any_ = pl.BlockSpec(memory_space=pl.ANY)
        vmem = pl.BlockSpec(memory_space=pltpu.VMEM)
        dma = pltpu.SemaphoreType.DMA
        return pl.pallas_call(
            functools.partial(kernel, n, tpn, heads, width, gates),
            out_shape=(
                jax.ShapeDtypeStruct((2, seqs, heads, width, width), BF16),
                jax.ShapeDtypeStruct((2, seqs, heads, width), F32),
                jax.ShapeDtypeStruct((2, seqs, heads), F32),
                jax.ShapeDtypeStruct((seqs, columns // tpn), BF16),
            ),
            in_specs=[any_, any_, any_, any_, vmem, vmem],
            out_specs=(any_, vmem, vmem, vmem),
            scratch_shapes=[
                pltpu.VMEM((seqs, length, depth), BF16),
                pltpu.VMEM(wkt.shape, BF16),
                pltpu.VMEM(wv.shape, BF16),
                pltpu.VMEM(wo.shape, BF16),
                pltpu.VMEM((2, seqs, heads, width, width), BF16),
                pltpu.VMEM((seqs, 1, heads * width), F32),
                pltpu.VMEM((gates, 128), F32),
                pltpu.VMEM((tpn, seqs, columns // tpn), F32),
                pltpu.VMEM((tpn, seqs, columns // tpn), F32),
                dma((3,)),
                dma((rounds,)),
                dma((rounds, n)),
                dma((rounds, n)),
                dma((rounds, tpn)),
                dma((rounds, tpn)),
                dma((2, seqs)),
                dma((tpn,)),
                dma((tpn,)),
            ],
            compiler_params=pltpu.CompilerParams(collective_id=0, has_side_effects=True),
            name="memories",
        )(prompt, wkt, wv, wo, bias, query)

    return jax.shard_map(
        body,
        mesh=mesh,
        in_specs=(
            P("gr", "sp", None),
            P(None, "tp", None),
            P(None, "tp", None),
            P(None, None, "tp"),
            P(None, None, "tp"),
            P(None, "tp"),
            P(None, "tp"),
            P(("gr", "sp"), "tp", None),
            P("tp", None, None),
        ),
        out_specs=(
            P(None, ("gr", "sp"), "tp", None, None),
            P(None, ("gr", "sp"), "tp", None),
            P(None, ("gr", "sp"), "tp"),
            P(("gr", "sp"), "tp"),
        ),
        check_vma=False,
    )
```

```python
import functools

import jax
import jax.numpy as jnp
from jax import lax
from jax.experimental import pallas as pl
from jax.experimental.pallas import tpu as pltpu
from jax.sharding import PartitionSpec as P

MESH = pl.DeviceIdType.MESH
F32 = jnp.float32
BF16 = jnp.bfloat16


def nt(a, b):
    return lax.dot_general(a, b, (((1,), (1,)), ((), ())), preferred_element_type=F32)


def kernel(
    n, tpn, heads, width, gates,
    prompt, wk_hbm, wv_hbm, wo_hbm, in_gate, forget_gate, in_bias, forget_bias, query,
    membuf, norm_out, stab_out, read_out,
    xbuf, raw, wkt, wv, wo, bias, hid, stabs, parts, got,
    wsem, lsem, ssem, rsem, fsend, frecv, xsend, xrecv,
):
    sp = lax.axis_index("sp")
    tp = lax.axis_index("tp")
    seqs, length, _ = xbuf.shape
    rounds = seqs // tpn
    block = length // n
    order = sorted(range(1, n), key=lambda k: abs(k - n / 2))

    barrier = pltpu.get_barrier_semaphore()
    for k in order:
        pl.semaphore_signal(
            barrier, inc=1, device_id={"sp": lax.rem(sp + k, n)}, device_id_type=MESH
        )
    for j in range(1, tpn):
        pl.semaphore_signal(
            barrier, inc=1, device_id={"tp": lax.rem(tp + j, tpn)}, device_id_type=MESH
        )

    weights = [
        pltpu.make_async_copy(wk_hbm, raw.at[0], wsem.at[0]),
        pltpu.make_async_copy(wv_hbm, raw.at[1], wsem.at[1]),
        pltpu.make_async_copy(wo_hbm, wo, wsem.at[2]),
    ]
    rows = pl.ds(pl.multiple_of(sp * block, block), block)

    def own(r):
        q = tp * rounds + r
        return pltpu.make_async_copy(prompt.at[sp * seqs + q], xbuf.at[q, rows], lsem.at[r])

    def send(r, k):
        q = tp * rounds + r
        dest = lax.rem(sp + k, n)
        return pltpu.make_async_remote_copy(
            src_ref=prompt.at[dest * seqs + q],
            dst_ref=xbuf.at[q, rows],
            send_sem=ssem.at[r, k],
            recv_sem=rsem.at[r, k],
            device_id={"sp": dest},
            device_id_type=MESH,
        )

    def forward(r, j):
        q = tp * rounds + r
        return pltpu.make_async_remote_copy(
            src_ref=xbuf.at[q],
            dst_ref=xbuf.at[q],
            send_sem=fsend.at[r, j],
            recv_sem=frecv.at[r, j],
            device_id={"tp": lax.rem(tp + j, tpn)},
            device_id_type=MESH,
        )

    for copy in weights:
        copy.start()
    for r in range(rounds):
        own(r).start()
    pl.semaphore_wait(barrier, n - 1 + tpn - 1)
    for r in range(rounds):
        for k in order:
            send(r, k).start()
    stabs[...] = jnp.zeros_like(stabs)
    key_rows = heads * width
    depth = wv.shape[0]

    def gate_rows(ref):
        pieces = [ref[g].astype(F32) for g in range(2)]
        if gates > 2 * heads:
            pieces.append(jnp.zeros((gates - 2 * heads, depth), F32))
        return jnp.concatenate(pieces, axis=0)

    wkt[key_rows:] = jnp.concatenate([gate_rows(in_gate), gate_rows(forget_gate)], axis=0).astype(BF16)
    line = lax.broadcasted_iota(jnp.int32, bias.shape, 0)
    column = jnp.zeros(bias.shape, F32)
    for base, ref in ((0, in_bias), (gates, forget_bias)):
        for g in range(2):
            for h in range(heads):
                column = jnp.where(line == base + g * heads + h, ref[g, h], column)
    bias[...] = column
    weights[0].wait()
    for d in range(0, depth, 128):
        wkt[:key_rows, d : d + 128] = raw[0, d : d + 128].reshape(128, key_rows).T
    weights[1].wait()
    wv[...] = raw[1].reshape(depth, key_rows)
    weights[2].wait()

    tri = (
        lax.broadcasted_iota(jnp.int32, (length, length), 0)
        <= lax.broadcasted_iota(jnp.int32, (length, length), 1)
    ).astype(F32)
    ahead = lax.broadcasted_iota(jnp.int32, (gates, length), 0) < heads
    lane = lax.broadcasted_iota(jnp.int32, (gates, stabs.shape[1]), 1)
    pick = lax.broadcasted_iota(jnp.int32, (16, length), 0)

    def compute(q):
        x = xbuf[q]
        kt = nt(wkt[...], x)
        values = jnp.dot(x, wv[...], preferred_element_type=F32).astype(BF16)
        pre = kt[key_rows:] + bias[...]
        keys = kt[:key_rows].astype(BF16)
        in_log, forget_pre = pre[:gates], pre[gates:]
        forget = jnp.minimum(forget_pre, 0.0) - jnp.log1p(jnp.exp(-jnp.abs(forget_pre)))
        running = jnp.dot(
            forget, tri, preferred_element_type=F32, precision=lax.Precision.HIGHEST
        )
        total = jnp.sum(forget, axis=1, keepdims=True)
        log_weight = in_log + jnp.where(ahead, total - running, running - forget)
        stable = jnp.maximum(total, jnp.max(log_weight, axis=1, keepdims=True))
        weight = jnp.exp(log_weight - stable) * width ** (-0.5)
        floor = jnp.maximum(jnp.exp(-stable), 1.0)
        stabs[...] = jnp.where(lane == q, stable, stabs[...])
        high = weight.astype(BF16).astype(F32)
        split = jnp.concatenate([high, weight - high], axis=0).astype(BF16)
        queries = query[q]
        for h in range(heads):
            head = keys[h * width : (h + 1) * width]
            head_f = head.astype(F32)
            w0, w1 = weight[h : h + 1], weight[heads + h : heads + h + 1]
            scores = jnp.dot(queries, head, preferred_element_type=F32)[h : h + 1]
            q0, q1 = scores * w0, scores * w1
            both = jnp.where(lax.rem(pick, 2) == 0, q0, q1)
            top = both.astype(BF16).astype(F32)
            tail = jnp.where(pick < 2, top, jnp.where(pick < 4, both - top, 0.0)).astype(BF16)
            lhs = jnp.concatenate(
                [(head_f * w0).astype(BF16), (head_f * w1).astype(BF16), tail], axis=0
            )
            res = jnp.dot(
                lhs, values[:, h * width : (h + 1) * width], preferred_element_type=F32
            )
            membuf[0, q, h] = res[:width].astype(BF16)
            membuf[1, q, h] = res[width : 2 * width].astype(BF16)
            normal = nt(split, head)
            normal = normal[:gates] + normal[gates:]
            norm_out[0, q, h : h + 1] = normal[h : h + 1]
            norm_out[1, q, h : h + 1] = normal[heads + h : heads + h + 1]
            last = res[2 * width :]
            d0 = jnp.abs(jnp.sum(q0, axis=1, keepdims=True))
            d1 = jnp.abs(jnp.sum(q1, axis=1, keepdims=True))
            f0, f1 = floor[h : h + 1], floor[heads + h : heads + h + 1]
            hid[q, :, h * width : (h + 1) * width] = (
                (last[0:1] + last[2:3]) / jnp.maximum(d0, f0)
                + (last[1:2] + last[3:4]) / jnp.maximum(d1, f1)
            )

    def turn(r, carry):
        own(r).wait()
        for k in order:
            send(r, k).wait_recv()
        for j in range(1, tpn):
            forward(r, j).start()
        compute(tp * rounds + r)
        for j in range(1, tpn):
            forward(r, j).wait_recv()
            compute(lax.rem(tp + tpn - j, tpn) * rounds + r)
        return carry

    lax.fori_loop(0, rounds, turn, 0)

    terms = jnp.dot(hid[:, 0, :].astype(BF16), wo[...], preferred_element_type=F32)
    share = terms.shape[1] // tpn
    for t in range(tpn):
        parts[t] = terms[:, t * share : (t + 1) * share]

    def give(j):
        peer = lax.rem(tp + j, tpn)
        return pltpu.make_async_remote_copy(
            src_ref=parts.at[peer],
            dst_ref=got.at[j],
            send_sem=xsend.at[j],
            recv_sem=xrecv.at[j],
            device_id={"tp": peer},
            device_id_type=MESH,
        )

    for j in range(1, tpn):
        give(j).start()
    for g in range(2):
        stab_out[g] = stabs[g * heads : (g + 1) * heads, :seqs]
    for r in range(rounds):
        for k in order:
            send(r, k).wait_send()
        for j in range(1, tpn):
            forward(r, j).wait_send()
    total = parts[tp]
    for j in range(1, tpn):
        give(j).wait()
        total = total + got[j]
    read_out[...] = total.astype(BF16)


def publish(count, *refs):
    sources, targets, sems = refs[:count], refs[count : 2 * count], refs[2 * count]
    copies = [
        pltpu.make_async_copy(a, b, sems.at[i]) for i, (a, b) in enumerate(zip(sources, targets))
    ]
    for copy in copies:
        copy.start()
    for copy in copies:
        copy.wait()


def solution(mesh):
    n, tpn = mesh.shape["sp"], mesh.shape["tp"]

    def body(prompt, w_key, w_value, w_in_gate, w_forget_gate, in_bias, forget_bias, query, w_out):
        depth, heads, width = w_key.shape
        seqs = prompt.shape[0] // n
        length = prompt.shape[1] * n
        rounds = seqs // tpn
        gates = -(-2 * heads // 8) * 8
        wo = w_out.reshape(heads * width, -1)
        columns = wo.shape[1]
        any_ = pl.BlockSpec(memory_space=pl.ANY)
        vmem = pl.BlockSpec(memory_space=pltpu.VMEM)
        smem = pl.BlockSpec(memory_space=pltpu.SMEM)
        dma = pltpu.SemaphoreType.DMA
        shapes = (
            ((2, seqs, heads, width, width), BF16),
            ((2, seqs, heads, width), F32),
            ((2, heads, seqs), F32),
            ((seqs, columns // tpn), BF16),
        )
        held = pl.pallas_call(
            functools.partial(kernel, n, tpn, heads, width, gates),
            out_shape=tuple(pltpu.VMEM(*shape) for shape in shapes),
            in_specs=[any_] * 4 + [vmem, vmem, smem, smem, vmem],
            out_specs=(vmem,) * 4,
            scratch_shapes=[
                pltpu.VMEM((seqs, length, depth), BF16),
                pltpu.VMEM((2, depth, heads, width), BF16),
                pltpu.VMEM((heads * width + 2 * gates, depth), BF16),
                pltpu.VMEM((depth, heads * width), BF16),
                pltpu.VMEM(wo.shape, BF16),
                pltpu.VMEM((2 * gates, length), F32),
                pltpu.VMEM((seqs, 1, heads * width), F32),
                pltpu.VMEM((gates, 128), F32),
                pltpu.VMEM((tpn, seqs, columns // tpn), F32),
                pltpu.VMEM((tpn, seqs, columns // tpn), F32),
                dma((3,)),
                dma((rounds,)),
                dma((rounds, n)),
                dma((rounds, n)),
                dma((rounds, tpn)),
                dma((rounds, tpn)),
                dma((tpn,)),
                dma((tpn,)),
            ],
            compiler_params=pltpu.CompilerParams(collective_id=0, has_side_effects=True),
            name="memories",
        )(
            prompt, w_key, w_value, wo,
            w_in_gate.transpose(0, 2, 1), w_forget_gate.transpose(0, 2, 1),
            in_bias, forget_bias, query,
        )
        memory, normal, stable, read = pl.pallas_call(
            functools.partial(publish, len(shapes)),
            out_shape=tuple(jax.ShapeDtypeStruct(*shape) for shape in shapes),
            in_specs=[vmem] * len(shapes),
            out_specs=(any_,) * len(shapes),
            scratch_shapes=[dma((len(shapes),))],
            name="outputs",
        )(*[pltpu.with_memory_space_constraint(a, pltpu.VMEM) for a in held])
        return memory, normal, stable.transpose(0, 2, 1), read

    return jax.shard_map(
        body,
        mesh=mesh,
        in_specs=(
            P("gr", "sp", None),
            P(None, "tp", None),
            P(None, "tp", None),
            P(None, None, "tp"),
            P(None, None, "tp"),
            P(None, "tp"),
            P(None, "tp"),
            P(("gr", "sp"), "tp", None),
            P("tp", None, None),
        ),
        out_specs=(
            P(None, ("gr", "sp"), "tp", None, None),
            P(None, ("gr", "sp"), "tp", None),
            P(None, ("gr", "sp"), "tp"),
            P(("gr", "sp"), "tp"),
        ),
        check_vma=False,
    )
```

```python
import functools

import jax
import jax.numpy as jnp
from jax import lax
from jax.experimental import pallas as pl
from jax.experimental.pallas import tpu as pltpu
from jax.sharding import PartitionSpec as P

MESH = pl.DeviceIdType.MESH
F32 = jnp.float32
BF16 = jnp.bfloat16


def nt(a, b):
    return lax.dot_general(a, b, (((1,), (1,)), ((), ())), preferred_element_type=F32)


def kernel(
    n, tpn, heads, width, gates,
    prompt, wk_hbm, wv_hbm, wo_hbm, ig_hbm, fg_hbm, ib_hbm, fb_hbm, q_hbm,
    membuf, norm_out, stab_out, read_out,
    in_gate, forget_gate, in_bias, forget_bias, query, xbuf, raw, wkt, wv, wo, bias, hid, stabs, parts, got,
    wsem, lsem, ssem, rsem, fsend, frecv, xsend, xrecv,
):
    sp = lax.axis_index("sp")
    tp = lax.axis_index("tp")
    seqs, length, _ = xbuf.shape
    rounds = seqs // tpn
    block = length // n
    order = sorted(range(1, n), key=lambda k: abs(k - n / 2))

    barrier = pltpu.get_barrier_semaphore()
    for k in order:
        pl.semaphore_signal(
            barrier, inc=1, device_id={"sp": lax.rem(sp + k, n)}, device_id_type=MESH
        )
    for j in range(1, tpn):
        pl.semaphore_signal(
            barrier, inc=1, device_id={"tp": lax.rem(tp + j, tpn)}, device_id_type=MESH
        )

    weights = [
        pltpu.make_async_copy(wk_hbm, raw.at[0], wsem.at[0]),
        pltpu.make_async_copy(wv_hbm, raw.at[1], wsem.at[1]),
        pltpu.make_async_copy(wo_hbm, wo, wsem.at[2]),
        pltpu.make_async_copy(ig_hbm, in_gate, wsem.at[3]),
        pltpu.make_async_copy(fg_hbm, forget_gate, wsem.at[4]),
        pltpu.make_async_copy(ib_hbm, in_bias, wsem.at[5]),
        pltpu.make_async_copy(fb_hbm, forget_bias, wsem.at[6]),
        pltpu.make_async_copy(q_hbm, query, wsem.at[7]),
    ]
    rows = pl.ds(pl.multiple_of(sp * block, block), block)

    def own(r):
        q = tp * rounds + r
        return pltpu.make_async_copy(prompt.at[sp * seqs + q], xbuf.at[q, rows], lsem.at[r])

    def send(r, k):
        q = tp * rounds + r
        dest = lax.rem(sp + k, n)
        return pltpu.make_async_remote_copy(
            src_ref=prompt.at[dest * seqs + q],
            dst_ref=xbuf.at[q, rows],
            send_sem=ssem.at[r, k],
            recv_sem=rsem.at[r, k],
            device_id={"sp": dest},
            device_id_type=MESH,
        )

    def forward(r, j):
        q = tp * rounds + r
        return pltpu.make_async_remote_copy(
            src_ref=xbuf.at[q],
            dst_ref=xbuf.at[q],
            send_sem=fsend.at[r, j],
            recv_sem=frecv.at[r, j],
            device_id={"tp": lax.rem(tp + j, tpn)},
            device_id_type=MESH,
        )

    for copy in weights:
        copy.start()
    for r in range(rounds):
        own(r).start()
    pl.semaphore_wait(barrier, n - 1 + tpn - 1)
    for r in range(rounds):
        for k in order:
            send(r, k).start()
    stabs[...] = jnp.zeros_like(stabs)
    for copy in weights[3:]:
        copy.wait()
    key_rows = heads * width
    depth = wv.shape[0]

    def gate_rows(ref):
        pieces = [ref[g].astype(F32) for g in range(2)]
        if gates > 2 * heads:
            pieces.append(jnp.zeros((gates - 2 * heads, depth), F32))
        return jnp.concatenate(pieces, axis=0)

    wkt[key_rows:] = jnp.concatenate([gate_rows(in_gate), gate_rows(forget_gate)], axis=0).astype(BF16)
    line = lax.broadcasted_iota(jnp.int32, bias.shape, 0)
    column = jnp.zeros(bias.shape, F32)
    for base, ref in ((0, in_bias), (gates, forget_bias)):
        for g in range(2):
            for h in range(heads):
                column = jnp.where(
                    line == base + g * heads + h, ref[g : g + 1, h : h + 1], column
                )
    bias[...] = column
    weights[0].wait()
    for d in range(0, depth, 128):
        wkt[:key_rows, d : d + 128] = raw[0, d : d + 128].reshape(128, key_rows).T
    weights[1].wait()
    wv[...] = raw[1].reshape(depth, key_rows)
    weights[2].wait()

    tri = (
        lax.broadcasted_iota(jnp.int32, (length, length), 0)
        <= lax.broadcasted_iota(jnp.int32, (length, length), 1)
    ).astype(BF16)
    ahead = lax.broadcasted_iota(jnp.int32, (gates, length), 0) < heads
    lane = lax.broadcasted_iota(jnp.int32, (gates, stabs.shape[1]), 1)
    pick = lax.broadcasted_iota(jnp.int32, (16, length), 0)

    def compute(q):
        x = xbuf[q]
        kt = nt(wkt[...], x)
        values = jnp.dot(x, wv[...], preferred_element_type=F32).astype(BF16)
        pre = kt[key_rows:] + bias[...]
        keys = kt[:key_rows].astype(BF16)
        in_log, forget_pre = pre[:gates], pre[gates:]
        forget = jnp.minimum(forget_pre, 0.0) - jnp.log1p(jnp.exp(-jnp.abs(forget_pre)))
        first = forget.astype(BF16).astype(F32)
        second = (forget - first).astype(BF16).astype(F32)
        third = forget - first - second
        pieces = jnp.concatenate([first, second, third, jnp.zeros_like(third)], axis=0)
        sums = jnp.dot(pieces.astype(BF16), tri, preferred_element_type=F32)
        running = sums[:gates] + sums[gates : 2 * gates] + sums[2 * gates : 3 * gates]
        total = running[:, length - 1 :]
        log_weight = in_log + jnp.where(ahead, total - running, running - forget)
        stable = jnp.maximum(total, jnp.max(log_weight, axis=1, keepdims=True))
        weight = jnp.exp(log_weight - stable) * width ** (-0.5)
        floor = jnp.maximum(jnp.exp(-stable), 1.0)
        stabs[...] = jnp.where(lane == q, stable, stabs[...])
        high = weight.astype(BF16).astype(F32)
        split = jnp.concatenate([high, weight - high], axis=0).astype(BF16)
        queries = query[q]
        for h in range(heads):
            head = keys[h * width : (h + 1) * width]
            head_f = head.astype(F32)
            w0, w1 = weight[h : h + 1], weight[heads + h : heads + h + 1]
            scores = jnp.dot(queries, head, preferred_element_type=F32)[h : h + 1]
            q0, q1 = scores * w0, scores * w1
            both = jnp.where(lax.rem(pick, 2) == 0, q0, q1)
            top = both.astype(BF16).astype(F32)
            tail = jnp.where(pick < 2, top, jnp.where(pick < 4, both - top, 0.0)).astype(BF16)
            lhs = jnp.concatenate(
                [(head_f * w0).astype(BF16), (head_f * w1).astype(BF16), tail], axis=0
            )
            res = jnp.dot(
                lhs, values[:, h * width : (h + 1) * width], preferred_element_type=F32
            )
            membuf[0, q, h] = res[:width].astype(BF16)
            membuf[1, q, h] = res[width : 2 * width].astype(BF16)
            normal = nt(split, head)
            normal = normal[:gates] + normal[gates:]
            norm_out[0, q, h : h + 1] = normal[h : h + 1]
            norm_out[1, q, h : h + 1] = normal[heads + h : heads + h + 1]
            last = res[2 * width :]
            d0 = jnp.abs(jnp.sum(q0, axis=1, keepdims=True))
            d1 = jnp.abs(jnp.sum(q1, axis=1, keepdims=True))
            f0, f1 = floor[h : h + 1], floor[heads + h : heads + h + 1]
            hid[q, :, h * width : (h + 1) * width] = (
                (last[0:1] + last[2:3]) / jnp.maximum(d0, f0)
                + (last[1:2] + last[3:4]) / jnp.maximum(d1, f1)
            )

    def turn(r, carry):
        own(r).wait()
        for k in order:
            send(r, k).wait_recv()
        for j in range(1, tpn):
            forward(r, j).start()
        compute(tp * rounds + r)
        for j in range(1, tpn):
            forward(r, j).wait_recv()
            compute(lax.rem(tp + tpn - j, tpn) * rounds + r)
        return carry

    lax.fori_loop(0, rounds, turn, 0)

    terms = jnp.dot(hid[:, 0, :].astype(BF16), wo[...], preferred_element_type=F32)
    share = terms.shape[1] // tpn
    for t in range(tpn):
        parts[t] = terms[:, t * share : (t + 1) * share]

    def give(j):
        peer = lax.rem(tp + j, tpn)
        return pltpu.make_async_remote_copy(
            src_ref=parts.at[peer],
            dst_ref=got.at[j],
            send_sem=xsend.at[j],
            recv_sem=xrecv.at[j],
            device_id={"tp": peer},
            device_id_type=MESH,
        )

    for j in range(1, tpn):
        give(j).start()
    for g in range(2):
        stab_out[g] = stabs[g * heads : (g + 1) * heads, :seqs]
    for r in range(rounds):
        for k in order:
            send(r, k).wait_send()
        for j in range(1, tpn):
            forward(r, j).wait_send()
    total = parts[tp]
    for j in range(1, tpn):
        give(j).wait()
        total = total + got[j]
    read_out[...] = total.astype(BF16)


def publish(count, *refs):
    sources, targets, sems = refs[:count], refs[count : 2 * count], refs[2 * count]
    copies = [
        pltpu.make_async_copy(a, b, sems.at[i]) for i, (a, b) in enumerate(zip(sources, targets))
    ]
    for copy in copies:
        copy.start()
    for copy in copies:
        copy.wait()


def solution(mesh):
    n, tpn = mesh.shape["sp"], mesh.shape["tp"]

    def body(prompt, w_key, w_value, w_in_gate, w_forget_gate, in_bias, forget_bias, query, w_out):
        depth, heads, width = w_key.shape
        seqs = prompt.shape[0] // n
        length = prompt.shape[1] * n
        rounds = seqs // tpn
        gates = -(-2 * heads // 8) * 8
        wo = w_out.reshape(heads * width, -1)
        columns = wo.shape[1]
        any_ = pl.BlockSpec(memory_space=pl.ANY)
        vmem = pl.BlockSpec(memory_space=pltpu.VMEM)
        dma = pltpu.SemaphoreType.DMA
        shapes = (
            ((2, seqs, heads, width, width), BF16),
            ((2, seqs, heads, width), F32),
            ((2, heads, seqs), F32),
            ((seqs, columns // tpn), BF16),
        )
        held = pl.pallas_call(
            functools.partial(kernel, n, tpn, heads, width, gates),
            out_shape=tuple(pltpu.VMEM(*shape) for shape in shapes),
            in_specs=[any_] * 9,
            out_specs=(vmem,) * 4,
            scratch_shapes=[
                pltpu.VMEM((2, heads, depth), BF16),
                pltpu.VMEM((2, heads, depth), BF16),
                pltpu.VMEM((2, heads), F32),
                pltpu.VMEM((2, heads), F32),
                pltpu.VMEM((seqs, heads, width), BF16),
                pltpu.VMEM((seqs, length, depth), BF16),
                pltpu.VMEM((2, depth, heads, width), BF16),
                pltpu.VMEM((heads * width + 2 * gates, depth), BF16),
                pltpu.VMEM((depth, heads * width), BF16),
                pltpu.VMEM(wo.shape, BF16),
                pltpu.VMEM((2 * gates, length), F32),
                pltpu.VMEM((seqs, 1, heads * width), F32),
                pltpu.VMEM((gates, 128), F32),
                pltpu.VMEM((tpn, seqs, columns // tpn), F32),
                pltpu.VMEM((tpn, seqs, columns // tpn), F32),
                dma((8,)),
                dma((rounds,)),
                dma((rounds, n)),
                dma((rounds, n)),
                dma((rounds, tpn)),
                dma((rounds, tpn)),
                dma((tpn,)),
                dma((tpn,)),
            ],
            compiler_params=pltpu.CompilerParams(collective_id=0, has_side_effects=True),
            name="memories",
        )(
            prompt, w_key, w_value, wo,
            w_in_gate.transpose(0, 2, 1), w_forget_gate.transpose(0, 2, 1),
            in_bias, forget_bias, query,
        )
        memory, normal, stable, read = pl.pallas_call(
            functools.partial(publish, len(shapes)),
            out_shape=tuple(jax.ShapeDtypeStruct(*shape) for shape in shapes),
            in_specs=[vmem] * len(shapes),
            out_specs=(any_,) * len(shapes),
            scratch_shapes=[dma((len(shapes),))],
            name="outputs",
        )(*[pltpu.with_memory_space_constraint(a, pltpu.VMEM) for a in held])
        return memory, normal, stable.transpose(0, 2, 1), read

    return jax.shard_map(
        body,
        mesh=mesh,
        in_specs=(
            P("gr", "sp", None),
            P(None, "tp", None),
            P(None, "tp", None),
            P(None, None, "tp"),
            P(None, None, "tp"),
            P(None, "tp"),
            P(None, "tp"),
            P(("gr", "sp"), "tp", None),
            P("tp", None, None),
        ),
        out_specs=(
            P(None, ("gr", "sp"), "tp", None, None),
            P(None, ("gr", "sp"), "tp", None),
            P(None, ("gr", "sp"), "tp"),
            P(("gr", "sp"), "tp"),
        ),
        check_vma=False,
    )
```

```python
import functools

import jax
import jax.numpy as jnp
from jax import lax
from jax.experimental import pallas as pl
from jax.experimental.pallas import tpu as pltpu
from jax.sharding import PartitionSpec as P

MESH = pl.DeviceIdType.MESH
F32 = jnp.float32
BF16 = jnp.bfloat16


def nt(a, b):
    return lax.dot_general(a, b, (((1,), (1,)), ((), ())), preferred_element_type=F32)


def kernel(
    n, tpn, heads, width, gates,
    prompt, wk_hbm, wv_hbm, wo_hbm, ig_hbm, fg_hbm, ib_hbm, fb_hbm, q_hbm,
    membuf, norm_out, stab_out, read_out,
    in_gate, forget_gate, in_bias, forget_bias, query, xbuf, raw, wkt, wv, wo, bias, hid, stabs, parts, got,
    wsem, lsem, ssem, rsem, fsend, frecv, xsend, xrecv,
):
    sp = lax.axis_index("sp")
    tp = lax.axis_index("tp")
    seqs, length, _ = xbuf.shape
    rounds = seqs // tpn
    block = length // n
    order = sorted(range(1, n), key=lambda k: abs(k - n / 2))

    barrier = pltpu.get_barrier_semaphore()
    for k in order:
        pl.semaphore_signal(
            barrier, inc=1, device_id={"sp": lax.rem(sp + k, n)}, device_id_type=MESH
        )
    for j in range(1, tpn):
        pl.semaphore_signal(
            barrier, inc=1, device_id={"tp": lax.rem(tp + j, tpn)}, device_id_type=MESH
        )

    weights = [
        pltpu.make_async_copy(wk_hbm, raw.at[0], wsem.at[0]),
        pltpu.make_async_copy(wv_hbm, raw.at[1], wsem.at[1]),
        pltpu.make_async_copy(wo_hbm, wo, wsem.at[2]),
        pltpu.make_async_copy(ig_hbm, in_gate, wsem.at[3]),
        pltpu.make_async_copy(fg_hbm, forget_gate, wsem.at[4]),
        pltpu.make_async_copy(ib_hbm, in_bias, wsem.at[5]),
        pltpu.make_async_copy(fb_hbm, forget_bias, wsem.at[6]),
        pltpu.make_async_copy(q_hbm, query, wsem.at[7]),
    ]
    rows = pl.ds(pl.multiple_of(sp * block, block), block)

    def own(r):
        q = tp * rounds + r
        return pltpu.make_async_copy(prompt.at[sp * seqs + q], xbuf.at[q, rows], lsem.at[r])

    def send(r, k):
        q = tp * rounds + r
        dest = lax.rem(sp + k, n)
        return pltpu.make_async_remote_copy(
            src_ref=prompt.at[dest * seqs + q],
            dst_ref=xbuf.at[q, rows],
            send_sem=ssem.at[r, k],
            recv_sem=rsem.at[r, k],
            device_id={"sp": dest},
            device_id_type=MESH,
        )

    def forward(r, j):
        q = tp * rounds + r
        return pltpu.make_async_remote_copy(
            src_ref=xbuf.at[q],
            dst_ref=xbuf.at[q],
            send_sem=fsend.at[r, j],
            recv_sem=frecv.at[r, j],
            device_id={"tp": lax.rem(tp + j, tpn)},
            device_id_type=MESH,
        )

    for copy in weights:
        copy.start()
    for r in range(rounds):
        own(r).start()
    pl.semaphore_wait(barrier, n - 1 + tpn - 1)
    for r in range(rounds):
        for k in order:
            send(r, k).start()
    stabs[...] = jnp.zeros_like(stabs)
    for copy in weights[3:]:
        copy.wait()
    key_rows = heads * width
    depth = wv.shape[0]

    def gate_rows(ref):
        pieces = [ref[g].astype(F32) for g in range(2)]
        if gates > 2 * heads:
            pieces.append(jnp.zeros((gates - 2 * heads, depth), F32))
        return jnp.concatenate(pieces, axis=0)

    wkt[key_rows:] = jnp.concatenate([gate_rows(in_gate), gate_rows(forget_gate)], axis=0).astype(BF16)
    line = lax.broadcasted_iota(jnp.int32, bias.shape, 0)
    column = jnp.zeros(bias.shape, F32)
    for base, ref in ((0, in_bias), (gates, forget_bias)):
        for g in range(2):
            for h in range(heads):
                column = jnp.where(
                    line == base + g * heads + h, ref[g : g + 1, h : h + 1], column
                )
    bias[...] = column
    weights[0].wait()
    for d in range(0, depth, 128):
        wkt[:key_rows, d : d + 128] = raw[0, d : d + 128].reshape(128, key_rows).T
    weights[1].wait()
    wv[...] = raw[1].reshape(depth, key_rows)
    weights[2].wait()

    tri = (
        lax.broadcasted_iota(jnp.int32, (length, length), 0)
        <= lax.broadcasted_iota(jnp.int32, (length, length), 1)
    ).astype(BF16)
    ahead = lax.broadcasted_iota(jnp.int32, (gates, length), 0) < heads
    lane = lax.broadcasted_iota(jnp.int32, (gates, stabs.shape[1]), 1)
    pick = lax.broadcasted_iota(jnp.int32, (16, length), 0)

    def project(q):
        x = xbuf[q]
        values = jnp.dot(x, wv[...], preferred_element_type=F32).astype(BF16)
        return nt(wkt[...], x), values

    def compute(q, kt, values):
        pre = kt[key_rows:] + bias[...]
        keys = kt[:key_rows].astype(BF16)
        in_log, forget_pre = pre[:gates], pre[gates:]
        forget = jnp.minimum(forget_pre, 0.0) - jnp.log1p(jnp.exp(-jnp.abs(forget_pre)))
        first = forget.astype(BF16).astype(F32)
        second = (forget - first).astype(BF16).astype(F32)
        third = forget - first - second
        pieces = jnp.concatenate([first, second, third, jnp.zeros_like(third)], axis=0)
        sums = jnp.dot(pieces.astype(BF16), tri, preferred_element_type=F32)
        running = sums[:gates] + sums[gates : 2 * gates] + sums[2 * gates : 3 * gates]
        total = running[:, length - 1 :]
        log_weight = in_log + jnp.where(ahead, total - running, running - forget)
        stable = jnp.maximum(total, jnp.max(log_weight, axis=1, keepdims=True))
        weight = jnp.exp(log_weight - stable) * width ** (-0.5)
        floor = jnp.maximum(jnp.exp(-stable), 1.0)
        stabs[...] = jnp.where(lane == q, stable, stabs[...])
        high = weight.astype(BF16).astype(F32)
        split = jnp.concatenate([high, weight - high], axis=0).astype(BF16)
        queries = query[q]
        for h in range(heads):
            head = keys[h * width : (h + 1) * width]
            head_f = head.astype(F32)
            w0, w1 = weight[h : h + 1], weight[heads + h : heads + h + 1]
            scores = jnp.dot(queries, head, preferred_element_type=F32)[h : h + 1]
            q0, q1 = scores * w0, scores * w1
            both = jnp.where(lax.rem(pick, 2) == 0, q0, q1)
            top = both.astype(BF16).astype(F32)
            tail = jnp.where(pick < 2, top, jnp.where(pick < 4, both - top, 0.0)).astype(BF16)
            lhs = jnp.concatenate(
                [(head_f * w0).astype(BF16), (head_f * w1).astype(BF16), tail], axis=0
            )
            res = jnp.dot(
                lhs, values[:, h * width : (h + 1) * width], preferred_element_type=F32
            )
            membuf[0, q, h] = res[:width].astype(BF16)
            membuf[1, q, h] = res[width : 2 * width].astype(BF16)
            normal = nt(split, head)
            normal = normal[:gates] + normal[gates:]
            norm_out[0, q, h : h + 1] = normal[h : h + 1]
            norm_out[1, q, h : h + 1] = normal[heads + h : heads + h + 1]
            last = res[2 * width :]
            d0 = jnp.abs(jnp.sum(q0, axis=1, keepdims=True))
            d1 = jnp.abs(jnp.sum(q1, axis=1, keepdims=True))
            f0, f1 = floor[h : h + 1], floor[heads + h : heads + h + 1]
            hid[q, :, h * width : (h + 1) * width] = (
                (last[0:1] + last[2:3]) / jnp.maximum(d0, f0)
                + (last[1:2] + last[3:4]) / jnp.maximum(d1, f1)
            )

    def turn(r, carry):
        own(r).wait()
        for k in order:
            send(r, k).wait_recv()
        for j in range(1, tpn):
            forward(r, j).start()
        before = (tp * rounds + r, *project(tp * rounds + r))
        for j in range(1, tpn):
            forward(r, j).wait_recv()
            q = lax.rem(tp + tpn - j, tpn) * rounds + r
            after = (q, *project(q))
            compute(*before)
            before = after
        compute(*before)
        return carry

    lax.fori_loop(0, rounds, turn, 0)

    terms = jnp.dot(hid[:, 0, :].astype(BF16), wo[...], preferred_element_type=F32)
    share = terms.shape[1] // tpn
    for t in range(tpn):
        parts[t] = terms[:, t * share : (t + 1) * share]

    def give(j):
        peer = lax.rem(tp + j, tpn)
        return pltpu.make_async_remote_copy(
            src_ref=parts.at[peer],
            dst_ref=got.at[j],
            send_sem=xsend.at[j],
            recv_sem=xrecv.at[j],
            device_id={"tp": peer},
            device_id_type=MESH,
        )

    for j in range(1, tpn):
        give(j).start()
    for g in range(2):
        stab_out[g] = stabs[g * heads : (g + 1) * heads, :seqs]
    for r in range(rounds):
        for k in order:
            send(r, k).wait_send()
        for j in range(1, tpn):
            forward(r, j).wait_send()
    total = parts[tp]
    for j in range(1, tpn):
        give(j).wait()
        total = total + got[j]
    read_out[...] = total.astype(BF16)


def publish(count, *refs):
    sources, targets, sems = refs[:count], refs[count : 2 * count], refs[2 * count]
    copies = [
        pltpu.make_async_copy(a, b, sems.at[i]) for i, (a, b) in enumerate(zip(sources, targets))
    ]
    for copy in copies:
        copy.start()
    for copy in copies:
        copy.wait()


def solution(mesh):
    n, tpn = mesh.shape["sp"], mesh.shape["tp"]

    def body(prompt, w_key, w_value, w_in_gate, w_forget_gate, in_bias, forget_bias, query, w_out):
        depth, heads, width = w_key.shape
        seqs = prompt.shape[0] // n
        length = prompt.shape[1] * n
        rounds = seqs // tpn
        gates = -(-2 * heads // 8) * 8
        wo = w_out.reshape(heads * width, -1)
        columns = wo.shape[1]
        any_ = pl.BlockSpec(memory_space=pl.ANY)
        vmem = pl.BlockSpec(memory_space=pltpu.VMEM)
        dma = pltpu.SemaphoreType.DMA
        shapes = (
            ((2, seqs, heads, width, width), BF16),
            ((2, seqs, heads, width), F32),
            ((2, heads, seqs), F32),
            ((seqs, columns // tpn), BF16),
        )
        held = pl.pallas_call(
            functools.partial(kernel, n, tpn, heads, width, gates),
            out_shape=tuple(pltpu.VMEM(*shape) for shape in shapes),
            in_specs=[any_] * 9,
            out_specs=(vmem,) * 4,
            scratch_shapes=[
                pltpu.VMEM((2, heads, depth), BF16),
                pltpu.VMEM((2, heads, depth), BF16),
                pltpu.VMEM((2, heads), F32),
                pltpu.VMEM((2, heads), F32),
                pltpu.VMEM((seqs, heads, width), BF16),
                pltpu.VMEM((seqs, length, depth), BF16),
                pltpu.VMEM((2, depth, heads, width), BF16),
                pltpu.VMEM((heads * width + 2 * gates, depth), BF16),
                pltpu.VMEM((depth, heads * width), BF16),
                pltpu.VMEM(wo.shape, BF16),
                pltpu.VMEM((2 * gates, length), F32),
                pltpu.VMEM((seqs, 1, heads * width), F32),
                pltpu.VMEM((gates, 128), F32),
                pltpu.VMEM((tpn, seqs, columns // tpn), F32),
                pltpu.VMEM((tpn, seqs, columns // tpn), F32),
                dma((8,)),
                dma((rounds,)),
                dma((rounds, n)),
                dma((rounds, n)),
                dma((rounds, tpn)),
                dma((rounds, tpn)),
                dma((tpn,)),
                dma((tpn,)),
            ],
            compiler_params=pltpu.CompilerParams(collective_id=0, has_side_effects=True),
            name="memories",
        )(
            prompt, w_key, w_value, wo,
            w_in_gate.transpose(0, 2, 1), w_forget_gate.transpose(0, 2, 1),
            in_bias, forget_bias, query,
        )
        memory, normal, stable, read = pl.pallas_call(
            functools.partial(publish, len(shapes)),
            out_shape=tuple(jax.ShapeDtypeStruct(*shape) for shape in shapes),
            in_specs=[vmem] * len(shapes),
            out_specs=(any_,) * len(shapes),
            scratch_shapes=[dma((len(shapes),))],
            name="outputs",
        )(*[pltpu.with_memory_space_constraint(a, pltpu.VMEM) for a in held])
        return memory, normal, stable.transpose(0, 2, 1), read

    return jax.shard_map(
        body,
        mesh=mesh,
        in_specs=(
            P("gr", "sp", None),
            P(None, "tp", None),
            P(None, "tp", None),
            P(None, None, "tp"),
            P(None, None, "tp"),
            P(None, "tp"),
            P(None, "tp"),
            P(("gr", "sp"), "tp", None),
            P("tp", None, None),
        ),
        out_specs=(
            P(None, ("gr", "sp"), "tp", None, None),
            P(None, ("gr", "sp"), "tp", None),
            P(None, ("gr", "sp"), "tp"),
            P(("gr", "sp"), "tp"),
        ),
        check_vma=False,
    )
```
